256 devices in a mesh: ep: 128 (over z, y, x), tp: 2 (over core).
Axes of the slice: x: 4, y: 4, z: 8, core: 2. Of those that a mesh axis runs over, the one named last changes fastest.
Arguments:
- tokens: bfloat16 [2048, 1024], P('ep'), may hold values from -6 to 6
- lengths: int32 [2048], P('ep'), may hold values from 1 to 1024, 1048576 in all
- routes: int32 [2048, 2], replicated, may hold values from 0 to 15, all different within a row; in each aligned block of 16 rows (0 to 15, 16 to 31, ...) at most 4 rows name the same one
- route_weights: float32 [2048, 2], replicated, may hold values from 0.1 to 1
- key_cache: bfloat16 [2048, 1024, 256], P('ep', None, 'tp'), may hold values from -6 to 6
- value_cache: bfloat16 [2048, 1024, 256], P('ep', None, 'tp'), may hold values from -6 to 6
- w_query: bfloat16 [1024, 1024], P(None, 'tp'), may hold values from -0.1875 to 0.1875
- w_key: bfloat16 [1024, 256], P(None, 'tp'), may hold values from -0.1875 to 0.1875
- w_value: bfloat16 [1024, 256], P(None, 'tp'), may hold values from -0.1875 to 0.1875
- w_out: bfloat16 [1024, 1024], P('tp'), may hold values from -0.1875 to 0.1875
- score_offset: float32 [16], P('tp'), may hold values from -9 to -3
- attn_gain: float32 [1024], replicated, may hold values from 0.1 to 1.9
- ffn_gain: float32 [1024], replicated, may hold values from 0.1 to 1.9
- w_gate: bfloat16 [1024, 114688], P(None, ('ep', 'tp')), may hold values from -0.1875 to 0.1875
- w_up: bfloat16 [1024, 114688], P(None, ('ep', 'tp')), may hold values from -0.1875 to 0.1875
- w_down: bfloat16 [114688, 1024], P(('ep', 'tp')), may hold values from -0.0625 to 0.0625
Outputs:
- layer_out: bfloat16 [2048, 1024], P('ep', 'tp')
- new_keys: bfloat16 [2048, 256], P('ep', 'tp')
- new_values: bfloat16 [2048, 256], P('ep', 'tp')
The draws below stay inside these ranges and needn't reach their ends.
Inputs may be any that keep to these rules, and one draw needn't show every extreme that they name: `routes`: each row names 2 different experts. Among the rows of one index of ep (aligned blocks of 16 rows) no expert is named by more than 4 rows, and in some block one expert is named by exactly 4 rows.
All inputs are finite; a program needn't handle non-finite values. No bound on the sum of `lengths` on one device may be relied on, other than what follows from the above.
Results may differ from the reference program's by a relative error of at most 0.0095.
Values may be sent and summed in bfloat16 or wider, within the bound.
A program may use at most 128 MiB of HBM per device.

```python
import math
import jax
import jax.numpy as jnp
import numpy as np
from jax import lax

D = 1024
HEADS = 16
KV_HEADS = 4
HEAD_DIM = 64
EXP_WIDTH = 7168
EXPERTS = 16
TOPK = 2
SEQ_DEV = 16
CTX = 1024
TOKENS = 2048
CAP = 4
N_EP = 128


def draw_score_offset(key, part):
    chooser = jax.random.fold_in(key, 11)
    slow_key = jax.random.fold_in(key, 12)
    fast_key = jax.random.fold_in(key, 13)
    slow_heads = jax.random.bernoulli(chooser, 0.5, (HEADS,))
    slow_values = jax.random.uniform(slow_key, (HEADS,), jnp.float32, -8.0, -7.0)
    fast_values = jax.random.uniform(fast_key, (HEADS,), jnp.float32, -4.0, -3.0)
    return jnp.where(slow_heads, slow_values, fast_values)


def block_levels(stream_key, dims, shards, low, largest):
    def one(position, blocks):
        steps = jax.random.uniform(jax.random.fold_in(jax.random.fold_in(stream_key, 6), position), (blocks,), jnp.float32, low / len(shards), largest / len(shards))
        return jnp.repeat(jnp.exp(steps), dims[position] // blocks).reshape((-1,) + (1,) * (len(dims) - position - 1))

    level = one(*shards[0])
    for cut in shards[1:]:
        level = level * one(*cut)
    return level


def length_profile(number_of, total, bound, slope):
    weights = [(1 << 20) // math.isqrt(standing ** slope) + 1 for standing in range(2, number_of + 1)]
    spare, holding = total - bound - (number_of - 1), [1] * (number_of - 1)
    while spare > 0:
        candidates = [i for i in range(number_of - 1) if holding[i] < bound]
        whole, remaining = sum([weights[i] for i in candidates]), spare
        for i in candidates:
            extra = min(bound - holding[i], max(1, remaining * weights[i] // whole), spare)
            holding[i] = holding[i] + extra
            spare = spare - extra
    return np.array([bound] + holding)


def uneven_parts(own_key, amount, total, limit, skew):
    if amount == 2:
        one = jax.random.randint(own_key, (), max(1, total - limit), min(limit, total - 1) + 1)
        return jnp.stack([one, total - one])
    sizes = jnp.asarray(length_profile(amount, total, limit, skew), jnp.int32)
    pairs = (amount - 1) // 2
    donor, receiver = sizes[1:1 + 2 * pairs:2], sizes[2:2 + 2 * pairs:2]
    slack = jnp.minimum(donor - 1, limit - receiver)
    shifted = jax.random.randint(jax.random.fold_in(own_key, 1), (pairs,), 0, 1 << 20) % (slack + 1)
    sizes = sizes.at[1:1 + 2 * pairs:2].set(donor - shifted).at[2:2 + 2 * pairs:2].set(receiver + shifted)
    return sizes[jax.random.permutation(jax.random.fold_in(own_key, 2), amount)]


def shared_out(key, own, number, rows, number_of, top, bound, lean):
    order = jax.random.permutation(key, number_of)
    heavy_load, common = portions_of(number_of, rows * top, bound, lean, True), portions_of(number_of, rows * top, bound, lean, False)
    places = jnp.arange(number_of)

    def named(sizes, turn):
        used = int((sizes > 0).sum())
        fixed = max(1, used // 4)
        shifted = fixed + (places - fixed + turn * (used - fixed)) % max(1, number_of - fixed)
        return jnp.zeros((number_of,), jnp.int32).at[order[jnp.where(places < fixed, places, shifted)]].set(jnp.asarray(sizes, jnp.int32))

    sizes = jnp.where(number % 4 == 0, named(heavy_load, number // 4), named(common, number - number // 4 - 1))
    mixed = jax.random.permutation(jax.random.fold_in(own, 3), number_of)
    source_of, taker = mixed[0:number_of // 2 * 2:2], mixed[1:number_of // 2 * 2:2]
    margin = jnp.minimum(sizes[source_of] - 1, bound - sizes[taker]) // 2
    margin = jnp.where((source_of == order[0]) | (taker == order[0]) | (sizes[taker] == 0), 0, jnp.maximum(margin, 0))
    shifted = jax.random.randint(jax.random.fold_in(own, 4), (number_of // 2,), 0, 1 << 20) % (margin + 1)
    sizes = sizes.at[source_of].add(-shifted).at[taker].add(shifted)
    members = jnp.searchsorted(jnp.cumsum(sizes), jnp.arange(rows * top), side="right").astype(jnp.int32)
    listing = members.reshape(top, rows).T
    listing = listing[jax.random.permutation(jax.random.fold_in(own, 1), rows)]
    turn = jax.random.randint(jax.random.fold_in(own, 2), (rows, 1), 0, top)
    return jnp.take_along_axis(listing, (jnp.arange(top)[None, :] + turn) % top, axis=1)


def portions_of(amount, total, bound, skew, full):
    portions = [(1 << 20) // math.isqrt(grade ** skew) + 1 for grade in range(1, amount + 1)]
    largest = bound if full else min(bound, max(-(-total // amount), total * portions[0] // sum(portions)))
    least = 1 if total - largest >= amount - 1 else 0
    given, surplus = [largest] + [least] * (amount - 1), total - largest - least * (amount - 1)
    while surplus > 0:
        free = [i for i in range(1, amount) if given[i] < largest] or [i for i in range(1, amount) if given[i] < bound]
        whole, budget = sum([portions[i] for i in free]), surplus
        for i in free:
            more = min(bound - given[i], max(1, budget * portions[i] // whole), surplus)
            given[i] = given[i] + more
            surplus = surplus - more
    return np.array(given)


def bell_draw(own_key, shape, scale, limit, pieces=(), kind=jnp.bfloat16):
    result = scale * jax.random.normal(own_key, shape, jnp.float32)
    if pieces:
        result = result * block_levels(own_key, shape, pieces, -0.22, 0.18)
    return jnp.clip(result, -limit, limit).astype(kind)


def setup_inputs(seed: int = 0) -> dict:
    arg_keys = jax.random.split(jax.random.key(seed), 17)
    tokens = bell_draw(arg_keys[0], (TOKENS, D), 1.0, 6.0, ((0, 128),))
    lengths = uneven_parts(arg_keys[1], TOKENS, TOKENS * CTX // 2, CTX, 2).astype(jnp.int32)
    routes_keys = jax.random.split(jax.random.fold_in(arg_keys[2], 1), TOKENS // SEQ_DEV)
    routes_turns = jax.random.permutation(jax.random.fold_in(arg_keys[2], 3), TOKENS // SEQ_DEV)
    routes = jax.vmap(lambda own, number: shared_out(jax.random.fold_in(arg_keys[2], 2), own, number, SEQ_DEV, EXPERTS, TOPK, CAP, 2))(routes_keys, routes_turns).reshape((TOKENS, TOPK))
    route_weights = jnp.clip(jax.random.uniform(arg_keys[3], (TOKENS, TOPK), jnp.float32, 0.1, 1.0), 0.1, 1.0)
    key_cache = bell_draw(arg_keys[4], (TOKENS, CTX, KV_HEADS * HEAD_DIM), 1.0, 6.0, ((0, 128), (2, 2)))
    value_cache = bell_draw(arg_keys[5], (TOKENS, CTX, KV_HEADS * HEAD_DIM), 1.0, 6.0, ((0, 128), (2, 2)))
    w_query = bell_draw(arg_keys[6], (D, HEADS * HEAD_DIM), D ** -0.5, 0.1875, ((1, 2),))
    w_key = bell_draw(arg_keys[7], (D, KV_HEADS * HEAD_DIM), D ** -0.5, 0.1875, ((1, 2),))
    w_value = bell_draw(arg_keys[8], (D, KV_HEADS * HEAD_DIM), D ** -0.5, 0.1875, ((1, 2),))
    w_out = bell_draw(arg_keys[9], (HEADS * HEAD_DIM, D), (HEADS * HEAD_DIM) ** -0.5, 0.1875, ((0, 2),))
    score_offset = draw_score_offset(jax.random.fold_in(arg_keys[16], 71), 0)
    attn_gain = jnp.clip(1.0 + 0.18 * jax.random.normal(arg_keys[11], (D,), jnp.float32), 0.1, 1.9)
    ffn_gain = jnp.clip(1.0 + 0.18 * jax.random.normal(arg_keys[12], (D,), jnp.float32), 0.1, 1.9)
    w_gate = bell_draw(arg_keys[13], (D, EXPERTS * EXP_WIDTH), D ** -0.5, 0.1875, ((1, 256),))
    w_up = bell_draw(arg_keys[14], (D, EXPERTS * EXP_WIDTH), D ** -0.5, 0.1875, ((1, 256),))
    w_down = bell_draw(arg_keys[15], (EXPERTS * EXP_WIDTH, D), EXP_WIDTH ** -0.5, 0.0625, ((0, 256),))
    return {"tokens": tokens, "lengths": lengths, "routes": routes, "route_weights": route_weights, "key_cache": key_cache, "value_cache": value_cache, "w_query": w_query, "w_key": w_key, "w_value": w_value, "w_out": w_out, "score_offset": score_offset, "attn_gain": attn_gain, "ffn_gain": ffn_gain, "w_gate": w_gate, "w_up": w_up, "w_down": w_down}


norm_eps = 1e-06

def rms_rows(values, gain_row):
    widened = values.astype(jnp.float32)
    scaled = widened * lax.rsqrt(lax.optimization_barrier(jnp.mean(widened * widened, axis=-1, keepdims=True)) + norm_eps)
    return (scaled * gain_row).astype(jnp.bfloat16)

def expert_rows(inputs, gate_cols, up_cols, down_rows):
    gate = jnp.dot(inputs, gate_cols, preferred_element_type=jnp.float32)
    upward = jnp.dot(inputs, up_cols, preferred_element_type=jnp.float32)
    hidden = (jax.nn.silu(gate) * upward).astype(jnp.bfloat16)
    return jnp.dot(hidden, down_rows, preferred_element_type=jnp.float32)

def reference(tokens, lengths, routes, route_weights, key_cache, value_cache, w_query, w_key, w_value, w_out, score_offset, attn_gain, ffn_gain, w_gate, w_up, w_down):
    normed = rms_rows(tokens, attn_gain)
    queries = jnp.dot(normed, w_query, preferred_element_type=jnp.float32).astype(jnp.bfloat16)
    new_keys = jnp.dot(normed, w_key, preferred_element_type=jnp.float32).astype(jnp.bfloat16)
    new_values = jnp.dot(normed, w_value, preferred_element_type=jnp.float32).astype(jnp.bfloat16)
    group_size = HEADS // KV_HEADS
    offsets = score_offset.reshape(KV_HEADS, group_size)[None, :, :, None]

    def attend(blocks):
        query_block, key_block, value_block, length_block = blocks
        count_rows = query_block.shape[0]
        query_heads = query_block.reshape(count_rows, KV_HEADS, group_size, HEAD_DIM).astype(jnp.float32)
        key_heads = key_block.reshape(count_rows, CTX, KV_HEADS, HEAD_DIM).astype(jnp.float32)
        value_heads = value_block.reshape(count_rows, CTX, KV_HEADS, HEAD_DIM).astype(jnp.float32)
        scores = jnp.einsum('bkgd,bskd->bkgs', query_heads, key_heads, precision=lax.Precision.HIGHEST) * HEAD_DIM ** (-0.5) + offsets
        valid = jnp.arange(CTX, dtype=jnp.int32)[None, None, None, :] < length_block[:, None, None, None]
        log_fail = jnp.where(valid, jax.nn.log_sigmoid(-scores), 0.0)
        after = lax.cumsum(log_fail, axis=3, reverse=True) - log_fail
        stick = jnp.where(valid, jnp.exp(jax.nn.log_sigmoid(scores) + after), 0.0).astype(jnp.bfloat16)
        output = jnp.einsum('bkgs,bskd->bkgd', stick.astype(jnp.float32), value_heads, precision=lax.Precision.HIGHEST)
        return output.astype(jnp.bfloat16).reshape(count_rows, HEADS * HEAD_DIM)
    attended = lax.map(attend, (queries.reshape(N_EP, SEQ_DEV, HEADS * HEAD_DIM), key_cache.reshape(N_EP, SEQ_DEV, CTX, KV_HEADS * HEAD_DIM), value_cache.reshape(N_EP, SEQ_DEV, CTX, KV_HEADS * HEAD_DIM), lengths.reshape(N_EP, SEQ_DEV)))
    attended = attended.reshape(TOKENS, HEADS * HEAD_DIM)
    per_half = HEADS * HEAD_DIM // 2
    running = tokens.astype(jnp.float32)
    for half_index in range(2):
        partial_part = jnp.dot(attended[:, half_index * per_half:(half_index + 1) * per_half], w_out[half_index * per_half:(half_index + 1) * per_half], preferred_element_type=jnp.float32)
        rounded = lax.optimization_barrier(partial_part.astype(jnp.bfloat16))
        running = running + rounded.astype(jnp.float32)
    middle = running.astype(jnp.bfloat16)
    moe_in = rms_rows(middle, ffn_gain)
    flat_routes = routes.reshape(-1)
    flat_weights = route_weights.reshape(-1)
    most_rows = N_EP * CAP

    def per_expert(mixture, expert):
        chosen = flat_routes == expert
        picked = jnp.nonzero(chosen, size=most_rows, fill_value=0)[0].astype(jnp.int32)
        filled_count = jnp.sum(chosen.astype(jnp.int32))
        filled = jnp.arange(most_rows, dtype=jnp.int32) < filled_count
        token_rows = (picked // TOPK).astype(jnp.int32)
        chosen_rows = moe_in[token_rows]
        start = (expert * EXP_WIDTH).astype(jnp.int32)
        gate_cols = lax.dynamic_slice_in_dim(w_gate, start, EXP_WIDTH, 1)
        up_cols = lax.dynamic_slice_in_dim(w_up, start, EXP_WIDTH, 1)
        down_rows = lax.dynamic_slice_in_dim(w_down, start, EXP_WIDTH, 0)
        outputs = expert_rows(chosen_rows, gate_cols, up_cols, down_rows)
        scale = jnp.where(filled, flat_weights[picked], 0.0)
        return (mixture.at[token_rows].add(scale[:, None] * outputs), None)
    mixture, _ = lax.scan(per_expert, jnp.zeros((TOKENS, D), jnp.float32), jnp.arange(EXPERTS, dtype=jnp.int32))
    layer_out = (middle.astype(jnp.float32) + mixture).astype(jnp.bfloat16)
    return (layer_out, new_keys, new_values)
```

```python
import jax
import jax.numpy as jnp
from jax import lax
from jax.experimental import pallas as pl
from jax.experimental.pallas import tpu as pltpu
from jax.sharding import PartitionSpec as P

HEAD_DIM = 64
SEQS = 16
CTX = 1024
HEADS = 8
BLOCK = 256
EPS = 1e-06
MESH = pl.DeviceIdType.MESH
F32 = jnp.float32
BF16 = jnp.bfloat16
HBM = pltpu.HBM
VMEM = pltpu.VMEM


def rms_rows(values, gain_row):
    scaled = values * lax.rsqrt(jnp.mean(values * values, axis=-1, keepdims=True) + EPS)
    return (scaled * gain_row).astype(BF16)


def dot(a, b):
    return jnp.dot(a, b, preferred_element_type=F32)


def dot_nt(a, b):
    return lax.dot_general(a, b, (((1,), (1,)), ((), ())), preferred_element_type=F32)


def iota(shape, dim):
    return lax.broadcasted_iota(jnp.int32, shape, dim)


def attend_kernel(
    tokens_hbm,
    gain_hbm,
    lengths_hbm,
    offset_hbm,
    routes_hbm,
    rweights_hbm,
    keys_hbm,
    values_hbm,
    wq_hbm,
    wk_hbm,
    wv_hbm,
    wo_hbm,
    part_ref,
    new_keys_ref,
    new_values_ref,
    pick_ref,
    weight_ref,
    tokens,
    gain,
    lengths,
    offset,
    routes,
    rweights,
    keys,
    values,
    wq,
    wk,
    wv,
    wo,
    turned,
    small_sem,
    weight_sem,
    key_sem,
    value_sem,
):
    ep = lax.axis_index("ep")
    lane_block = pl.multiple_of((ep // 8) * 128, 128)
    small = [
        pltpu.make_async_copy(tokens_hbm, tokens, small_sem.at[0]),
        pltpu.make_async_copy(gain_hbm, gain, small_sem.at[1]),
        pltpu.make_async_copy(lengths_hbm, lengths, small_sem.at[2]),
        pltpu.make_async_copy(offset_hbm, offset, small_sem.at[3]),
        pltpu.make_async_copy(routes_hbm.at[:, pl.ds(lane_block, 128)], routes, small_sem.at[4]),
        pltpu.make_async_copy(rweights_hbm.at[:, pl.ds(lane_block, 128)], rweights, small_sem.at[5]),
    ]
    weights = [
        pltpu.make_async_copy(wq_hbm, wq, weight_sem.at[0]),
        pltpu.make_async_copy(wk_hbm, wk, weight_sem.at[1]),
        pltpu.make_async_copy(wv_hbm, wv, weight_sem.at[2]),
        pltpu.make_async_copy(wo_hbm, wo, weight_sem.at[3]),
    ]
    key_copies = [
        pltpu.make_async_copy(keys_hbm.at[pl.ds(2 * p, 2)], keys.at[pl.ds(2 * p, 2)], key_sem.at[p])
        for p in range(8)
    ]
    value_copies = [
        pltpu.make_async_copy(values_hbm.at[pl.ds(2 * p, 2)], values.at[pl.ds(2 * p, 2)], value_sem.at[p])
        for p in range(8)
    ]
    for copy in small[:2] + weights[:1] + small[2:] + key_copies + weights[1:3] + value_copies + weights[3:]:
        copy.start()

    for copy in small[4:]:
        copy.wait()
    row = iota((128, 128), 0)
    lane = iota((128, 128), 1)
    mine = (lane // 16) == (ep % 8)
    first = jnp.logical_and(routes[0:1, :] == row // 8, mine)
    second = jnp.logical_and(routes[1:2, :] == row // 8, mine)
    named = jnp.logical_or(first, second)
    earlier = dot(named.astype(F32).astype(BF16), (row < lane).astype(F32).astype(BF16))
    chosen = jnp.logical_and(named, earlier == (row % 4).astype(F32))
    pick_ref[...] = chosen.astype(F32).astype(BF16)
    share = jnp.where(first, rweights[0:1, :], rweights[1:2, :])
    turned[...] = jnp.transpose(jnp.where(chosen, share, 0.0))
    weight_ref[...] = turned[pl.ds(pl.multiple_of((ep % 8) * 16, 16), 16), :]

    small[0].wait()
    small[1].wait()
    normed = rms_rows(tokens[...].astype(F32), gain[...])
    weights[0].wait()
    queries = dot(normed, wq[...])
    low = iota((SEQS, 128), 1) < HEAD_DIM
    by_head = []
    for h in range(HEADS):
        tile = queries[:, 128 * (h // 2) : 128 * (h // 2) + 128]
        if h % 2 != h // 4:
            tile = pltpu.roll(tile, HEAD_DIM, 1)
        by_head.append(jnp.where(low if h < 4 else jnp.logical_not(low), tile, 0.0))
    by_head = jnp.concatenate(by_head, axis=0).astype(BF16)
    to_seq = jnp.logical_and(row // 8 == lane % 16, row % 8 == lane // 16).astype(F32).astype(BF16)
    to_head = jnp.logical_and(row // 16 == lane % 8, row % 16 == lane // 8).astype(F32).astype(BF16)
    by_seq = dot(to_seq, by_head)
    wide = []
    for p in range(8):
        left = jnp.where(row // 8 == 2 * p, by_seq, 0.0).astype(BF16)
        right = jnp.where(row // 8 == 2 * p + 1, by_seq, 0.0).astype(BF16)
        wide.append(jnp.concatenate([left, right], axis=1))

    small[2].wait()
    small[3].wait()
    lane1 = iota((1, 128), 1)
    limit = jnp.zeros((1, 128), jnp.int32)
    for b in range(SEQS):
        limit = jnp.where(lane1 // 8 == b, lengths[b], limit)
    shift = jnp.zeros((1, 128), F32)
    for h in range(HEADS):
        shift = jnp.where(lane1 % 8 == h, offset[h], shift)

    upper = (iota((BLOCK, BLOCK), 1) >= iota((BLOCK, BLOCK), 0)).astype(F32).astype(BF16)
    for copy in key_copies:
        copy.wait()
    carry = jnp.zeros((1, 128), F32)
    sticks = [None] * (CTX // BLOCK)
    for i in reversed(range(CTX // BLOCK)):
        rows = slice(i * BLOCK, (i + 1) * BLOCK)
        scores = jnp.zeros((BLOCK, 128), F32)
        for p in range(8):
            pair = jnp.concatenate([keys[2 * p, rows, :], keys[2 * p + 1, rows, :]], axis=1)
            scores = scores + dot_nt(pair, wide[p])
        z = scores * HEAD_DIM ** (-0.5) + shift
        valid = iota((BLOCK, 128), 0) + i * BLOCK < limit
        fail = jnp.where(valid, -(jnp.maximum(z, 0.0) + jnp.log1p(jnp.exp(-jnp.abs(z)))), 0.0)
        high = fail.astype(BF16)
        rest = (fail - high.astype(F32)).astype(BF16)
        total = dot(upper, high) + dot(upper, rest) + carry
        carry = total[0:1, :]
        stick = jnp.where(valid, jnp.exp(z + total), 0.0)
        sticks[i] = jnp.transpose(stick).astype(BF16)

    weights[1].wait()
    new_keys_ref[...] = dot(normed, wk[...]).astype(BF16)
    weights[2].wait()
    new_values_ref[...] = dot(normed, wv[...]).astype(BF16)

    gathered = []
    top = iota((16, 128), 0) < 8
    for p in range(8):
        value_copies[p].wait()
        both = jnp.zeros((16, 256), F32)
        for i in range(CTX // BLOCK):
            rows = slice(i * BLOCK, (i + 1) * BLOCK)
            pair = jnp.concatenate([values[2 * p, rows, :], values[2 * p + 1, rows, :]], axis=1)
            both = both + dot(sticks[i][16 * p : 16 * p + 16, :], pair)
        gathered.append(jnp.where(top, both[:, :128], both[:, 128:]))
    gathered = jnp.concatenate(gathered, axis=0).astype(BF16)
    gathered = dot(to_head, gathered)
    tiles = []
    for p in range(4):
        pieces = []
        for h in (2 * p, 2 * p + 1):
            piece = gathered[16 * h : 16 * h + 16, :]
            if h % 2 != h // 4:
                piece = pltpu.roll(piece, HEAD_DIM, 1)
            pieces.append(piece)
        tiles.append(jnp.where(low, pieces[0], pieces[1]))
    attended = jnp.concatenate(tiles, axis=1).astype(BF16)
    weights[3].wait()
    part_ref[...] = dot(attended, wo[...]).astype(BF16)


def attend(tokens, lengths, routes, route_weights, key_cache, value_cache, wq, wk, wv, wo, offset, gain):
    hbm = pl.BlockSpec(memory_space=HBM)
    vmem = pl.BlockSpec(memory_space=VMEM)
    return pl.pallas_call(
        attend_kernel,
        name="attend",
        out_shape=(
            jax.ShapeDtypeStruct((SEQS, 1024), BF16),
            jax.ShapeDtypeStruct((SEQS, 128), BF16),
            jax.ShapeDtypeStruct((SEQS, 128), BF16),
            jax.ShapeDtypeStruct((128, 128), BF16),
            jax.ShapeDtypeStruct((16, 128), F32),
        ),
        in_specs=[hbm] * 12,
        out_specs=[vmem] * 5,
        scratch_shapes=[
            VMEM((SEQS, 1024), BF16),
            VMEM((1, 1024), F32),
            pltpu.SMEM((SEQS,), jnp.int32),
            pltpu.SMEM((HEADS,), F32),
            VMEM((2, 128), jnp.int32),
            VMEM((2, 128), F32),
            VMEM((SEQS, CTX, 128), BF16),
            VMEM((SEQS, CTX, 128), BF16),
            VMEM((1024, 512), BF16),
            VMEM((1024, 128), BF16),
            VMEM((1024, 128), BF16),
            VMEM((512, 1024), BF16),
            VMEM((128, 128), F32),
            pltpu.SemaphoreType.DMA((6,)),
            pltpu.SemaphoreType.DMA((4,)),
            pltpu.SemaphoreType.DMA((8,)),
            pltpu.SemaphoreType.DMA((8,)),
        ],
        compiler_params=pltpu.CompilerParams(vmem_limit_bytes=40 * 1024 * 1024),
        cost_estimate=pl.CostEstimate(flops=2 * 10**9, bytes_accessed=11 * 2**20, transcendentals=400000),
    )(
        tokens,
        gain.reshape(1, 1024),
        lengths,
        offset,
        routes.T,
        route_weights.T,
        key_cache,
        value_cache,
        wq,
        wk,
        wv,
        wo,
    )


def expert_kernel(
    part_ref,
    tokens_ref,
    gain_ref,
    pick_ref,
    weight_ref,
    wg_hbm,
    wu_hbm,
    wd_hbm,
    out_ref,
    wg,
    wu,
    wd,
    other_part,
    outgoing,
    arrived,
    rows,
    own_sums,
    pair_send,
    pair_recv,
    up_send,
    up_recv,
    back_send,
    back_recv,
    weight_sem,
    part_sem,
    out_send_sem,
    out_recv_sem,
    ring_send_sem,
    ring_recv_sem,
    twin_send_sem,
    twin_recv_sem,
    pair_send_sem,
    pair_recv_sem,
    up_send_sem,
    up_recv_sem,
    back_send_sem,
    back_recv_sem,
):
    ep = lax.axis_index("ep")
    c = lax.axis_index("tp")
    x = ep % 4
    y = (ep // 4) % 4
    z = ep // 16

    def at(zz, yy, xx):
        return {"ep": (zz * 4 + yy) * 4 + xx, "tp": c}

    twin = {"ep": ep, "tp": 1 - c}
    right = at(z, y, (x + 1) % 4)
    left = at(z, y, (x + 3) % 4)
    across = at(z, y + 1 - 2 * (y % 2), x)

    def there(dz, f):
        return at((z + dz) % 8, (3 - y) if f else y, x)

    def back(dz, f):
        return at((z + 8 - dz) % 8, (3 - y) if f else y, x)

    far_first = [(dz, f) for dz in (4, 3, 5, 2, 6, 1, 7, 0) for f in (1, 0) if (dz, f) != (0, 0)]

    loads = [
        pltpu.make_async_copy(wg_hbm, wg, weight_sem.at[0]),
        pltpu.make_async_copy(wu_hbm, wu, weight_sem.at[1]),
        pltpu.make_async_copy(wd_hbm, wd, weight_sem.at[2]),
    ]
    for load in loads:
        load.start()

    barrier = pltpu.get_barrier_semaphore()
    for device in [there(dz, f) for dz, f in far_first] + [right, left, across, twin]:
        pl.semaphore_signal(barrier, inc=1, device_id=device, device_id_type=MESH)
    pl.semaphore_wait(barrier, 19)

    started = []

    def send(src, dst, send_sem, recv_sem, device):
        copy = pltpu.make_async_remote_copy(
            src_ref=src, dst_ref=dst, send_sem=send_sem, recv_sem=recv_sem, device_id=device, device_id_type=MESH
        )
        copy.start()
        started.append(copy)

    def arrival(dst, recv_sem):
        pltpu.make_async_remote_copy(
            src_ref=dst, dst_ref=dst, send_sem=recv_sem, recv_sem=recv_sem, device_id=twin, device_id_type=MESH
        ).wait_recv()

    send(part_ref, other_part, part_sem.at[0], part_sem.at[1], twin)
    arrival(other_part, part_sem.at[1])
    middle = tokens_ref[...].astype(F32) + (part_ref[...].astype(F32) + other_part[...].astype(F32))
    middle = middle.astype(BF16).astype(F32)
    moe_in = rms_rows(middle, gain_ref[...])
    moe_half = jnp.where(c == 0, moe_in[:, :512].astype(F32), moe_in[:, 512:].astype(F32)).astype(BF16)

    pick = pick_ref[...].astype(F32)
    half_row = (iota((128, 128), 0) // 4) % 2
    pick_wide = jnp.concatenate(
        [jnp.where(half_row == 0, pick, 0.0).astype(BF16), jnp.where(half_row == 1, pick, 0.0).astype(BF16)], axis=1
    )
    tall = jnp.concatenate([moe_half[:, :256]] * 8 + [moe_half[:, 256:]] * 8, axis=0)
    outgoing[...] = dot(pick_wide, tall).astype(BF16).reshape(16, 8, 256)
    for dz, f in far_first:
        n = 2 * dz + f
        expert = 2 * ((z + dz) % 8) + (y // 2 + f) % 2
        send(outgoing.at[expert], arrived.at[n], out_send_sem.at[n], out_recv_sem.at[n], there(dz, f))
    own_expert = 2 * z + y // 2
    arrived[0] = outgoing[own_expert]
    for dz, f in reversed(far_first):
        n = 2 * dz + f
        arrival(arrived.at[n], out_recv_sem.at[n])

    pool = arrived[...].reshape(128, 256)
    to_row = iota((64, 128), 0)
    from_row = iota((64, 128), 1)
    gather_left = (from_row == (to_row // 4) * 8 + to_row % 4).astype(F32).astype(BF16)
    gather_right = (from_row == (to_row // 4) * 8 + 4 + to_row % 4).astype(F32).astype(BF16)
    rows[0, c] = jnp.concatenate([dot(gather_left, pool), dot(gather_right, pool)], axis=1).astype(BF16)

    def pass_on(block, number, device, to_block, part=None):
        src, dst = rows.at[block, c], rows.at[to_block, c]
        if part is not None:
            src, dst = src.at[pl.ds(32 * part, 32)], dst.at[pl.ds(32 * part, 32)]
        slot = 8 if part == 1 else to_block
        send(src, dst, ring_send_sem.at[number], ring_recv_sem.at[slot], device)

    def share(block):
        send(rows.at[block, c], rows.at[block, c], twin_send_sem.at[block], twin_recv_sem.at[block], twin)

    def have(block):
        if block == 2:
            for part in range(2):
                arrival(rows.at[2, c].at[pl.ds(32 * part, 32)], ring_recv_sem.at[8 if part else 2])
        else:
            arrival(rows.at[block, c], ring_recv_sem.at[block])

    pass_on(0, 0, across, 4)
    pass_on(0, 1, right, 1)
    pass_on(0, 2, left, 3)
    share(0)
    have(4)
    pass_on(4, 3, right, 5)
    pass_on(4, 4, left, 7)
    share(4)
    have(1)
    pass_on(1, 5, right, 2, part=0)
    share(1)
    have(3)
    pass_on(3, 6, left, 2, part=1)
    share(3)

    def run(block_a, block_b):
        for block in (block_a, block_b):
            arrival(rows.at[block, 1 - c], twin_recv_sem.at[block])
        left_in = jnp.concatenate([rows[block_a, 0], rows[block_b, 0]], axis=0)
        right_in = jnp.concatenate([rows[block_a, 1], rows[block_b, 1]], axis=0)
        gate = dot_nt(left_in, wg[:, :512]) + dot_nt(right_in, wg[:, 512:])
        upward = dot_nt(left_in, wu[:, :512]) + dot_nt(right_in, wu[:, 512:])
        hidden = (gate / (1.0 + jnp.exp(-gate)) * upward).astype(BF16)
        outs = dot(hidden, wd[...])
        mine = jnp.where(c == 0, outs[:, :512], outs[:, 512:])
        theirs = jnp.where(c == 0, outs[:, 512:], outs[:, :512]).astype(BF16)
        for k, block in enumerate((block_a, block_b)):
            own_sums[block] = mine[64 * k : 64 * k + 64]
            pair_send[block] = theirs[64 * k : 64 * k + 64]
            send(pair_send.at[block], pair_recv.at[block], pair_send_sem.at[block], pair_recv_sem.at[block], twin)

    for load in loads:
        load.wait()
    run(0, 4)
    have(2)
    pass_on(2, 7, across, 6)
    share(2)
    run(1, 3)
    have(5)
    share(5)
    have(7)
    share(7)
    have(6)
    share(6)
    run(5, 7)
    run(2, 6)

    def chip_sum(block):
        arrival(pair_recv.at[block], pair_recv_sem.at[block])
        return own_sums[block] + pair_recv[block].astype(F32)

    def give(number, value, device):
        up_send[number] = value.astype(BF16)
        send(up_send.at[number], up_recv.at[number], up_send_sem.at[number], up_recv_sem.at[number], device)

    def taken(number):
        arrival(up_recv.at[number], up_recv_sem.at[number])
        return up_recv[number].astype(F32)

    give(0, chip_sum(5), left)
    give(1, chip_sum(7), right)
    give(2, chip_sum(6), across)
    far = chip_sum(2) + taken(2)
    up_send[3] = far.astype(BF16)
    for part, device in ((0, left), (1, right)):
        piece = pl.ds(32 * part, 32)
        send(
            up_send.at[3].at[piece],
            up_recv.at[3].at[piece],
            up_send_sem.at[3 + part],
            up_recv_sem.at[3 + part],
            device,
        )
    give(5, chip_sum(4) + taken(0) + taken(1), across)
    for part in range(2):
        arrival(up_recv.at[3].at[pl.ds(32 * part, 32)], up_recv_sem.at[3 + part])
    sum_1, sum_3 = chip_sum(1), chip_sum(3)
    give(6, jnp.concatenate([sum_1[:32] + up_recv[3, :32].astype(F32), sum_1[32:]], axis=0), left)
    give(7, jnp.concatenate([sum_3[:32], sum_3[32:] + up_recv[3, 32:].astype(F32)], axis=0), right)
    result = chip_sum(0) + taken(5) + taken(6) + taken(7)

    result = result.astype(BF16)
    to_pool = iota((128, 64), 0)
    from_slot = iota((128, 64), 1)
    spread = to_pool // 8 * 4 + to_pool % 4 == from_slot
    left_half = (to_pool // 4) % 2 == 0
    spread_left = jnp.logical_and(spread, left_half).astype(F32).astype(BF16)
    spread_right = jnp.logical_and(spread, jnp.logical_not(left_half)).astype(F32).astype(BF16)
    pool = dot(spread_left, result[:, :256]) + dot(spread_right, result[:, 256:])
    back_send[...] = pool.astype(BF16).reshape(16, 8, 256)
    for dz, f in far_first:
        n = 2 * dz + f
        send(back_send.at[n], back_recv.at[own_expert], back_send_sem.at[n], back_recv_sem.at[n], back(dz, f))
    back_recv[own_expert] = back_send[0]
    for dz, f in reversed(far_first):
        n = 2 * dz + f
        expert = 2 * ((z + dz) % 8) + (y // 2 + f) % 2
        arrival(back_recv.at[expert], back_recv_sem.at[n])
    pool = back_recv[...].reshape(128, 256)
    weight = weight_ref[...]
    column_half = (iota((16, 128), 1) // 4) % 2
    mixture = []
    for k in range(2):
        part = jnp.where(column_half == k, weight, 0.0)
        high = part.astype(BF16)
        mixture.append(dot(high, pool) + dot((part - high.astype(F32)).astype(BF16), pool))
    own_middle = jnp.where(c == 0, middle[:, :512], middle[:, 512:])
    out_ref[...] = (own_middle + jnp.concatenate(mixture, axis=1)).astype(BF16)
    for copy in started:
        copy.wait_send()


def experts(part, tokens, gain, pick, weight, w_gate, w_up, w_down):
    hbm = pl.BlockSpec(memory_space=HBM)
    vmem = pl.BlockSpec(memory_space=VMEM)
    dma = pltpu.SemaphoreType.DMA
    return pl.pallas_call(
        expert_kernel,
        name="experts",
        out_shape=jax.ShapeDtypeStruct((SEQS, 512), BF16),
        in_specs=[vmem] * 5 + [hbm] * 3,
        out_specs=vmem,
        scratch_shapes=[
            VMEM((448, 1024), BF16),
            VMEM((448, 1024), BF16),
            VMEM((448, 1024), BF16),
            VMEM((SEQS, 1024), BF16),
            VMEM((16, 8, 256), BF16),
            VMEM((16, 8, 256), BF16),
            VMEM((8, 2, 64, 512), BF16),
            VMEM((8, 64, 512), F32),
            VMEM((8, 64, 512), BF16),
            VMEM((8, 64, 512), BF16),
            VMEM((8, 64, 512), BF16),
            VMEM((8, 64, 512), BF16),
            VMEM((16, 8, 256), BF16),
            VMEM((16, 8, 256), BF16),
            dma((3,)),
            dma((2,)),
            dma((16,)),
            dma((16,)),
            dma((8,)),
            dma((9,)),
            dma((8,)),
            dma((8,)),
            dma((8,)),
            dma((8,)),
            dma((8,)),
            dma((8,)),
            dma((16,)),
            dma((16,)),
        ],
        compiler_params=pltpu.CompilerParams(
            collective_id=0, has_side_effects=True, vmem_limit_bytes=32 * 1024 * 1024
        ),
        cost_estimate=pl.CostEstimate(flops=2 * 10**9, bytes_accessed=3 * 2**20, transcendentals=300000),
    )(part, tokens, gain.reshape(1, 1024), pick, weight, w_gate.T, w_up.T, w_down)


def shards(
    tokens,
    lengths,
    routes,
    route_weights,
    key_cache,
    value_cache,
    w_query,
    w_key,
    w_value,
    w_out,
    score_offset,
    attn_gain,
    ffn_gain,
    w_gate,
    w_up,
    w_down,
):
    part, new_keys, new_values, pick, weight = attend(
        tokens,
        lengths,
        routes,
        route_weights,
        key_cache,
        value_cache,
        w_query,
        w_key,
        w_value,
        w_out,
        score_offset,
        attn_gain,
    )
    layer_out = experts(part, tokens, ffn_gain, pick, weight, w_gate, w_up, w_down)
    return (layer_out, new_keys, new_values)


def solution(mesh):
    in_specs = (
        P("ep", None),
        P("ep"),
        P(),
        P(),
        P("ep", None, "tp"),
        P("ep", None, "tp"),
        P(None, "tp"),
        P(None, "tp"),
        P(None, "tp"),
        P("tp", None),
        P("tp"),
        P(),
        P(),
        P(None, ("ep", "tp")),
        P(None, ("ep", "tp")),
        P(("ep", "tp"), None),
    )
    out_specs = (P("ep", "tp"), P("ep", "tp"), P("ep", "tp"))
    return jax.shard_map(shards, mesh=mesh, in_specs=in_specs, out_specs=out_specs, check_vma=False)
```
